32 devices in a mesh: fs: 8 (over z, y), tp: 4 (over x, core).
Axes of the slice: x: 2, y: 2, z: 4, core: 2. Of those that a mesh axis runs over, the one named last changes fastest.
Arguments:
- latent_in: bfloat16 [24576, 512], P('fs'), may hold values from -6 to 6
- query_cot: bfloat16 [24576, 1536], P('fs', 'tp'), may hold values from -6 to 6
- attn_out: bfloat16 [24576, 1024], P('fs'), may hold values from -6 to 6
- mix_cot: bfloat16 [24576, 2048], P('fs', 'tp'), may hold values from -6 to 6
- query_weight: float32 [512, 1536], P('fs', 'tp'), may hold values from -0.25 to 0.25
- output_weight: float32 [1024, 2048], P('fs', 'tp'), may hold values from -0.1875 to 0.1875
- query_factor: bfloat16 [512, 256], P('fs'), may hold values from -0.25 to 0.25
- output_factor: bfloat16 [1024, 256], P('fs'), may hold values from -0.1875 to 0.1875
- query_mean: float32 [256, 1536], P('fs', 'tp'), may hold values from -3 to 3
- query_square: float32 [256, 1536], P('fs', 'tp'), may hold values from 0.05 to 1
- output_mean: float32 [256, 2048], P('fs', 'tp'), may hold values from -3 to 3
- output_square: float32 [256, 2048], P('fs', 'tp'), may hold values from 0.05 to 1
Outputs:
- step_query: float32 [512, 1536], P('fs', 'tp')
- step_output: float32 [1024, 2048], P('fs', 'tp')
- new_query: float32 [512, 1536], P('fs', 'tp')
- new_output: float32 [1024, 2048], P('fs', 'tp')
- copy_query: bfloat16 [512, 1536], P(None, 'tp')
- copy_output: bfloat16 [1024, 2048], P(None, 'tp')
- query_mean_new: float32 [256, 1536], P('fs', 'tp')
- query_square_new: float32 [256, 1536], P('fs', 'tp')
- output_mean_new: float32 [256, 2048], P('fs', 'tp')
- output_square_new: float32 [256, 2048], P('fs', 'tp')
The draws below stay inside these ranges and needn't reach their ends.
All inputs are finite; a program needn't handle non-finite values.
Results may differ from the reference program's by a relative error of at most 0.0085.
Values may be sent and summed in bfloat16 or wider, within the bound.
A program may use at most 64 MiB of HBM per device.

```python
import math
import jax
import jax.numpy as jnp
from jax import lax

D = 2048
Q_RANK = 512
RANK = 256
QCOLS = 1536
HV = 1024
TOKENS = 24576


def level_of(key, extent, cuts, smallest, top_value):
    loudness, own = 1.0, jax.random.fold_in(key, 6)
    for axis_at, blocks in cuts:
        draws = jnp.exp(jax.random.uniform(jax.random.fold_in(own, axis_at), (blocks,), jnp.float32, smallest / len(cuts), top_value / len(cuts)))
        loudness = loudness * jnp.repeat(draws, extent[axis_at] // blocks).reshape([-1 if axis == axis_at else 1 for axis in range(len(extent))])
    return loudness


def normal_values(rng, extent, width, limit, shards=(), held_as=jnp.bfloat16):
    factor_of = level_of(rng, extent, shards, -0.22, 0.18) if shards else 1.0
    values = jax.random.normal(rng, extent, jnp.float32) * width * factor_of
    return jnp.minimum(jnp.maximum(values, -limit), limit).astype(held_as)


def setup_inputs(seed: int = 0) -> dict:
    key_of = jax.random.split(jax.random.key(seed), 13)
    latent_in = normal_values(key_of[0], (TOKENS, Q_RANK), 1.0, 6.0, ((0, 8),))
    query_cot = normal_values(key_of[1], (TOKENS, QCOLS), 1.0, 6.0, ((0, 8), (1, 4)))
    attn_out = normal_values(key_of[2], (TOKENS, HV), 1.0, 6.0, ((0, 8),))
    mix_cot = normal_values(key_of[3], (TOKENS, D), 1.0, 6.0, ((0, 8), (1, 4)))
    query_weight = normal_values(key_of[4], (Q_RANK, QCOLS), Q_RANK ** -0.5, 0.25, ((0, 8), (1, 4)), jnp.float32)
    output_weight = normal_values(key_of[5], (HV, D), HV ** -0.5, 0.1875, ((0, 8), (1, 4)), jnp.float32)
    query_factor = normal_values(key_of[6], (Q_RANK, RANK), Q_RANK ** -0.5, 0.25, ((0, 8),))
    output_factor = normal_values(key_of[7], (HV, RANK), HV ** -0.5, 0.1875, ((0, 8),))
    query_mean = normal_values(key_of[8], (RANK, QCOLS), 0.5, 3.0, ((0, 8), (1, 4)), jnp.float32)
    query_square = jnp.clip(jnp.exp(math.log(1.0) - 2.9957323 * jax.random.uniform(key_of[9], (RANK, QCOLS), jnp.float32) ** level_of(key_of[9], (RANK, QCOLS), ((0, 8), (1, 4)), -0.2, 0.2)), 0.05, 1.0)
    output_mean = normal_values(key_of[10], (RANK, D), 0.5, 3.0, ((0, 8), (1, 4)), jnp.float32)
    output_square = jnp.clip(jnp.exp(math.log(1.0) - 2.9957323 * jax.random.uniform(key_of[11], (RANK, D), jnp.float32) ** level_of(key_of[11], (RANK, D), ((0, 8), (1, 4)), -0.2, 0.2)), 0.05, 1.0)
    return {"latent_in": latent_in, "query_cot": query_cot, "attn_out": attn_out, "mix_cot": mix_cot, "query_weight": query_weight, "output_weight": output_weight, "query_factor": query_factor, "output_factor": output_factor, "query_mean": query_mean, "query_square": query_square, "output_mean": output_mean, "output_square": output_square}


def over_rows(left, right):
    return lax.dot_general(left, right, (((0,), (0,)), ((), ())), preferred_element_type=jnp.float32)

def exact_dot(left, right):
    return jnp.dot(left, right, precision=lax.Precision.HIGHEST, preferred_element_type=jnp.float32)

def moments(mean, square, low):
    mean_new = 0.8 * mean + 0.2 * low
    square_new = 0.9 * square + 0.1 * low * low
    return (mean_new, square_new, mean_new / jnp.sqrt(square_new))

def reference(latent_in, query_cot, attn_out, mix_cot, query_weight, output_weight, query_factor, output_factor, query_mean, query_square, output_mean, output_square):
    inv_root = 1.0 / math.sqrt(latent_in.shape[0])
    grad_query = over_rows(latent_in, query_cot) * inv_root
    grad_output = over_rows(attn_out, mix_cot) * inv_root
    factor_query = query_factor.astype(jnp.float32)
    factor_output = output_factor.astype(jnp.float32)
    low_query = exact_dot(factor_query.T, grad_query)
    low_output = exact_dot(factor_output.T, grad_output)
    mean_q, square_q, direction_q = moments(query_mean, query_square, low_query)
    mean_o, square_o, direction_o = moments(output_mean, output_square, low_output)
    scale_q = 1.0 / jnp.sqrt(jnp.mean(direction_q * direction_q) + 0.25)
    scale_o = 1.0 / jnp.sqrt(jnp.mean(direction_o * direction_o) + 0.25)
    step_q = exact_dot(factor_query, direction_q) * scale_q
    step_o = exact_dot(factor_output, direction_o) * scale_o
    new_q = query_weight - 0.02 * step_q
    new_o = output_weight - 0.02 * step_o
    return (step_q, step_o, new_q, new_o, new_q.astype(jnp.bfloat16), new_o.astype(jnp.bfloat16), mean_q, square_q, mean_o, square_o)
```

```python
import functools
import math

import jax
import jax.numpy as jnp
from jax import lax
from jax.experimental import pallas as pl
from jax.experimental.pallas import tpu as pltpu
from jax.sharding import PartitionSpec as P

MESH = pl.DeviceIdType.MESH
BF16 = jnp.bfloat16
F32 = jnp.float32
CHUNKS = 4


def grid_of(count):
    inner = max(d for d in range(1, count + 1) if count % d == 0 and d * d <= count)
    return count // inner, inner


def copies_of(nz, ny, nt):
    n = nz * ny
    per_gather = (nz - 1) + nz * (ny - 1)
    return per_gather + ny + 4 * per_gather + 2 * (nz + ny - 2) + (nt - 1) + (n - 1)


def over_rows(left, right):
    return lax.dot_general(left, right, (((0,), (0,)), ((), ())), preferred_element_type=F32)


def fused_kernel(
    nz, ny, nt, inv_root,
    latent_hbm, cot_hbm, attn_hbm, mix_hbm,
    wq_ref, wo_ref, fq_hbm, fo_hbm, qm_ref, qs_ref, om_ref, os_ref,
    fac, wq_all, wo_all, dq_all, do_all, low_q, low_o, total,
    latent, cot, attn, mix, grad_q, grad_o,
    part_q, part_o, yin_q, yin_o, acc_q, acc_o, zout_q, zout_o, zin_q, zin_o,
    tile_tp, tile_fs,
    load_sem, fac_sem, send_sem, recv_sem,
):
    n = nz * ny
    f = lax.axis_index("fs")
    t = lax.axis_index("tp")
    z, y = f // ny, f % ny
    half_cols = fac.shape[-1] // 2
    half = pl.ds(pl.multiple_of((t % 2) * half_cols, half_cols), half_cols)
    twin = t + 1 - 2 * (t % 2)
    rq = fq_hbm.shape[0]
    tokens = latent_hbm.shape[0]
    step = tokens // CHUNKS

    def load(k, pair, sem):
        rows = pl.ds(pl.multiple_of(k * step, step), step)
        return [
            pltpu.make_async_copy(src.at[rows, :], dst.at[rows, :], load_sem.at[k, sem + i])
            for i, (src, dst) in enumerate(pair)
        ]

    pair_o = ((attn_hbm, attn), (mix_hbm, mix))
    pair_q = ((latent_hbm, latent), (cot_hbm, cot))
    own = [
        pltpu.make_async_copy(fq_hbm.at[:, half], fac.at[z, y, pl.ds(0, rq), half], fac_sem.at[0]),
        pltpu.make_async_copy(
            fo_hbm.at[:, half], fac.at[z, y, pl.ds(rq, fo_hbm.shape[0]), half], fac_sem.at[1]
        ),
    ]
    for c in own:
        c.start()
    for k in range(CHUNKS):
        for c in load(k, pair_o, 0):
            c.start()
    for k in range(CHUNKS):
        for c in load(k, pair_q, 2):
            c.start()

    barrier = pltpu.get_barrier_semaphore()
    for d in range(1, n):
        pl.semaphore_signal(barrier, inc=1, device_id={"fs": (f + d) % n}, device_id_type=MESH)
    for d in range(1, nt):
        pl.semaphore_signal(barrier, inc=1, device_id={"tp": (t + d) % nt}, device_id_type=MESH)

    wq_all[z, y] = wq_ref[...].astype(BF16)
    wo_all[z, y] = wo_ref[...].astype(BF16)
    for c in own:
        c.wait()
    pl.semaphore_wait(barrier, n - 1 + nt - 1)

    started = []

    def send(src, dst, device):
        k = len(started)
        c = pltpu.make_async_remote_copy(
            src_ref=src, dst_ref=dst, send_sem=send_sem.at[k], recv_sem=recv_sem.at[k],
            device_id=device, device_id_type=MESH,
        )
        c.start()
        started.append(c)
        return c

    def to_z(d):
        return {"fs": ((z + d) % nz) * ny + y}

    def to_y(d):
        return {"fs": z * ny + (y + d) % ny}

    def z_send(block, ds):
        return {d: send(block(z), block(z), to_z(d)) for d in ds}

    def y_send(block, back):
        zz = (z + nz - back) % nz
        return [send(block(zz), block(zz), to_y(d)) for d in range(1, ny)]

    fac_block = lambda zz: fac.at[zz, y, :, half]
    wq_block = lambda zz: wq_all.at[zz, y]
    wo_block = lambda zz: wo_all.at[zz, y]
    dq_block = lambda zz: dq_all.at[zz, y]
    do_block = lambda zz: do_all.at[zz, y]

    far = range(1, nz)
    fac_z = z_send(fac_block, far)
    fac_y = y_send(fac_block, 0)
    early = far[: max(1, len(far) - 1)]
    w_z = {}
    for d in early:
        w_z[d] = (send(wo_block(z), wo_block(z), to_z(d)), send(wq_block(z), wq_block(z), to_z(d)))

    grad_o[...] = jnp.zeros_like(grad_o)
    grad_q[...] = jnp.zeros_like(grad_q)

    def product(k, pair, sem, out):
        for c in load(k, pair, sem):
            c.wait()
        rows = pl.ds(pl.multiple_of(k * step, step), step)
        out[...] += over_rows(pair[1][1][rows, :], pair[0][1][rows, :])

    @pl.loop(0, CHUNKS // 2)
    def _(k):
        product(k, pair_o, 0, grad_o)

    for d in far:
        fac_z[d].wait_recv()
        fac_y += y_send(fac_block, d)
    swap = [send(fac.at[:, y, :, half], fac.at[:, y, :, half], {"tp": twin})]

    @pl.loop(CHUNKS // 2, CHUNKS)
    def _(k):
        product(k, pair_o, 0, grad_o)

    for c in fac_y:
        c.wait_recv()
    for d in range(1, ny):
        other = fac.at[:, (y + ny - d) % ny, :, half]
        swap.append(send(other, other, {"tp": twin}))

    @pl.loop(0, CHUNKS)
    def _(k):
        product(k, pair_q, 2, grad_q)

    for c in swap:
        c.wait_recv()

    rank = fac.shape[-1]
    block = rank // n

    def project(lo, hi, grad, part):
        factor = fac[:, :, lo:hi, :].reshape(n * (hi - lo), rank)
        g = grad[...]
        top = g.astype(BF16)
        rest = (g - top.astype(F32)).astype(BF16)
        dims = (((0,), (1,)), ((), ()))
        low = lax.dot_general(factor, top, dims, preferred_element_type=F32)
        low += lax.dot_general(factor, rest, dims, preferred_element_type=F32)
        low *= inv_root
        for i in range(nz):
            for j in range(ny):
                at = (i * ny + j) * block
                part[i, j] = low[at:at + block, :]

    matrices = (
        (rq, fac.shape[2], grad_o, part_o, yin_o, acc_o, zout_o, zin_o),
        (0, rq, grad_q, part_q, yin_q, acc_q, zout_q, zin_q),
    )
    y_in = []
    for lo, hi, grad, part, yin, acc, zout, zin in matrices:
        project(lo, hi, grad, part)
        copies = []
        for d in range(1, ny):
            yy = (y + d) % ny
            acc_send = yin.at[d - 1]
            for i in range(nz):
                yin[ny - 1 + d - 1, i] = part[i, yy].astype(BF16)
            copies.append(send(yin.at[ny - 1 + d - 1], acc_send, to_y(d)))
        y_in.append(copies)

    z_in = []
    for (lo, hi, grad, part, yin, acc, zout, zin), copies in zip(matrices, y_in):
        for i in range(nz):
            acc[i] = part[i, y]
        for d, c in enumerate(copies):
            c.wait_recv()
            for i in range(nz):
                acc[i] += yin[d, i].astype(F32)
        copies = []
        for d in far:
            zout[d - 1] = acc[(z + d) % nz].astype(BF16)
            copies.append(send(zout.at[d - 1], zin.at[d - 1], to_z(d)))
        z_in.append(copies)

    for d in far:
        if d not in w_z:
            w_z[d] = (send(wo_block(z), wo_block(z), to_z(d)), send(wq_block(z), wq_block(z), to_z(d)))
    w_y = y_send(wo_block, 0) + y_send(wq_block, 0)

    def forward_weights(d):
        w_z[d][0].wait_recv()
        w_z[d][1].wait_recv()
        return y_send(wo_block, d) + y_send(wq_block, d)

    w_y += forward_weights(1) if nz > 1 else []

    sides = (
        (matrices[0], z_in[0], om_ref, os_ref, low_o, do_all, 1),
        (matrices[1], z_in[1], qm_ref, qs_ref, low_q, dq_all, 0),
    )
    d_z = []
    d_y = []
    for (_, _, _, _, _, acc, _, zin), copies, mean_ref, square_ref, low_ref, d_all, slot in sides:
        low = acc[z]
        for d, c in zip(far, copies):
            c.wait_recv()
            low += zin[d - 1].astype(F32)
        low_ref[...] = low
        mean_new = 0.8 * mean_ref[...] + 0.2 * low
        square_new = 0.9 * square_ref[...] + 0.1 * low * low
        direction = mean_new / jnp.sqrt(square_new)
        d_all[z, y] = direction.astype(BF16)
        tile_tp[0, slot] = jnp.broadcast_to(jnp.sum(direction * direction), tile_tp.shape[2:])
        where = lambda zz, d_all=d_all: d_all.at[zz, y]
        d_z.append((where, z_send(where, far)))
        d_y += y_send(where, 0)

    tiles = [
        send(tile_tp.at[0], tile_tp.at[d], {"tp": (t + d) % nt}) for d in range(1, nt)
    ]
    for c in tiles:
        c.wait_recv()
    tile_fs[0] = jnp.sum(tile_tp[...], axis=0)
    tiles = [
        send(tile_fs.at[0], tile_fs.at[d], {"fs": (f + d) % n}) for d in range(1, n)
    ]
    for d in far:
        for where, copies in d_z:
            copies[d].wait_recv()
            d_y += y_send(where, d)
    for d in far[1:]:
        w_y += forward_weights(d)
    for c in tiles:
        c.wait_recv()
    total[...] = jnp.sum(tile_fs[...], axis=0)
    for c in d_y + w_y:
        c.wait_recv()
    for c in started:
        c.wait_send()


def on_device(
    nz, ny, nt,
    latent_in, query_cot, attn_out, mix_cot, query_weight, output_weight,
    query_factor, output_factor, query_mean, query_square, output_mean, output_square,
):
    n = nz * ny
    tokens = latent_in.shape[0]
    inv_root = 1.0 / math.sqrt(tokens * n)
    rq, cq = query_weight.shape
    ro, co = output_weight.shape
    rank = query_factor.shape[1]
    block = rank // n
    vmem = pl.BlockSpec(memory_space=pltpu.VMEM)
    hbm = pl.BlockSpec(memory_space=pl.ANY)
    copies = copies_of(nz, ny, nt)
    fac, wq, wo, dq, do, low_q, low_o, total = pl.pallas_call(
        functools.partial(fused_kernel, nz, ny, nt, inv_root),
        name="moment_exchange",
        in_specs=[hbm] * 4 + [vmem] * 2 + [hbm] * 2 + [vmem] * 4,
        out_specs=[vmem] * 8,
        out_shape=[
            jax.ShapeDtypeStruct((nz, ny, rq + ro, rank), BF16),
            jax.ShapeDtypeStruct((nz, ny, rq, cq), BF16),
            jax.ShapeDtypeStruct((nz, ny, ro, co), BF16),
            jax.ShapeDtypeStruct((nz, ny, block, cq), BF16),
            jax.ShapeDtypeStruct((nz, ny, block, co), BF16),
            jax.ShapeDtypeStruct((block, cq), F32),
            jax.ShapeDtypeStruct((block, co), F32),
            jax.ShapeDtypeStruct((2, 8, 128), F32),
        ],
        scratch_shapes=[
            pltpu.VMEM(latent_in.shape, BF16),
            pltpu.VMEM(query_cot.shape, BF16),
            pltpu.VMEM(attn_out.shape, BF16),
            pltpu.VMEM(mix_cot.shape, BF16),
            pltpu.VMEM((cq, n * rq), F32),
            pltpu.VMEM((co, n * ro), F32),
            pltpu.VMEM((nz, ny, block, cq), F32),
            pltpu.VMEM((nz, ny, block, co), F32),
            pltpu.VMEM((2 * max(ny - 1, 1), nz, block, cq), BF16),
            pltpu.VMEM((2 * max(ny - 1, 1), nz, block, co), BF16),
            pltpu.VMEM((nz, block, cq), F32),
            pltpu.VMEM((nz, block, co), F32),
            pltpu.VMEM((max(nz - 1, 1), block, cq), BF16),
            pltpu.VMEM((max(nz - 1, 1), block, co), BF16),
            pltpu.VMEM((max(nz - 1, 1), block, cq), BF16),
            pltpu.VMEM((max(nz - 1, 1), block, co), BF16),
            pltpu.VMEM((nt, 2, 8, 128), F32),
            pltpu.VMEM((n, 2, 8, 128), F32),
            pltpu.SemaphoreType.DMA((CHUNKS, 4)),
            pltpu.SemaphoreType.DMA((2,)),
            pltpu.SemaphoreType.DMA((copies,)),
            pltpu.SemaphoreType.DMA((copies,)),
        ],
        compiler_params=pltpu.CompilerParams(
            collective_id=0, has_side_effects=True, vmem_limit_bytes=60 * 1024 * 1024
        ),
    )(
        latent_in, query_cot, attn_out, mix_cot, query_weight, output_weight,
        query_factor, output_factor, query_mean, query_square, output_mean, output_square,
    )

    def finish(factor, factor_all, direction, weight, weight_all, mean, square, low, slot):
        mean_new = 0.8 * mean + 0.2 * low
        square_new = 0.9 * square + 0.1 * low * low
        cols = weight.shape[1]
        scale = 1.0 / jnp.sqrt(total[slot, 0, 0] / (rank * cols * nt) + 0.25)
        direction = direction.reshape(rank, cols)
        step = jnp.dot(factor, direction, preferred_element_type=F32) * scale
        new = weight - 0.02 * step
        full = jnp.dot(factor_all.reshape(-1, rank), direction, preferred_element_type=F32) * scale
        copy = (weight_all.reshape(-1, cols).astype(F32) - 0.02 * full).astype(BF16)
        return step, new, copy, mean_new, square_new

    step_q, new_q, copy_q, mean_q, square_q = finish(
        query_factor, fac[:, :, :rq], dq, query_weight, wq, query_mean, query_square, low_q, 0
    )
    step_o, new_o, copy_o, mean_o, square_o = finish(
        output_factor, fac[:, :, rq:], do, output_weight, wo, output_mean, output_square, low_o, 1
    )
    return (step_q, step_o, new_q, new_o, copy_q, copy_o, mean_q, square_q, mean_o, square_o)


def solution(mesh):
    nz, ny = grid_of(mesh.shape["fs"])
    rows, both, cols = P("fs", None), P("fs", "tp"), P(None, "tp")
    return jax.shard_map(
        functools.partial(on_device, nz, ny, mesh.shape["tp"]),
        mesh=mesh,
        in_specs=(rows, both, rows, both, both, both, rows, rows, both, both, both, both),
        out_specs=(both, both, both, both, cols, cols, both, both, both, both),
        check_vma=False,
    )
```

```python
import functools
import math

import jax
import jax.numpy as jnp
from jax import lax
from jax.experimental import pallas as pl
from jax.experimental.pallas import tpu as pltpu
from jax.sharding import PartitionSpec as P

MESH = pl.DeviceIdType.MESH
BF16 = jnp.bfloat16
F32 = jnp.float32
CHUNKS = 4


def grid_of(count):
    inner = max(d for d in range(1, count + 1) if count % d == 0 and d * d <= count)
    return count // inner, inner


def copies_of(nz, ny, nt):
    n = nz * ny
    per_gather = (nz - 1) + nz * (ny - 1)
    return per_gather + ny + 4 * per_gather + 2 * (nz + ny - 2) + (nt - 1) + (n - 1)


def over_rows(left, right):
    return lax.dot_general(left, right, (((0,), (0,)), ((), ())), preferred_element_type=F32)


def fused_kernel(
    nz, ny, nt, inv_root,
    latent_hbm, cot_hbm, attn_hbm, mix_hbm,
    wq_ref, wo_ref, fq_hbm, fo_hbm, qm_ref, qs_ref, om_ref, os_ref,
    fac, wq_all, wo_all, dq_all, do_all, low_q, low_o, total,
    latent, cot, attn, mix, grad_q, grad_o,
    part_q, part_o, yin_q, yin_o, acc_q, acc_o, zout_q, zout_o, zin_q, zin_o,
    tile_tp, tile_fs,
    load_sem, fac_sem, send_sem, recv_sem,
):
    n = nz * ny
    f = lax.axis_index("fs")
    t = lax.axis_index("tp")
    z, y = f // ny, f % ny
    half_cols = fac.shape[-1] // 2
    half = pl.ds(pl.multiple_of((t % 2) * half_cols, half_cols), half_cols)
    twin = t + 1 - 2 * (t % 2)
    rq = fq_hbm.shape[0]
    tokens = latent_hbm.shape[0]
    step = tokens // CHUNKS

    def load(k, pair, sem):
        rows = pl.ds(pl.multiple_of(k * step, step), step)
        return [
            pltpu.make_async_copy(src.at[rows, :], dst.at[rows, :], load_sem.at[k, sem + i])
            for i, (src, dst) in enumerate(pair)
        ]

    pair_o = ((attn_hbm, attn), (mix_hbm, mix))
    pair_q = ((latent_hbm, latent), (cot_hbm, cot))
    own = [
        pltpu.make_async_copy(fq_hbm.at[:, half], fac.at[z, y, pl.ds(0, rq), half], fac_sem.at[0]),
        pltpu.make_async_copy(
            fo_hbm.at[:, half], fac.at[z, y, pl.ds(rq, fo_hbm.shape[0]), half], fac_sem.at[1]
        ),
    ]
    for c in own:
        c.start()
    for k in range(CHUNKS):
        for c in load(k, pair_o, 0):
            c.start()
    for k in range(CHUNKS):
        for c in load(k, pair_q, 2):
            c.start()

    barrier = pltpu.get_barrier_semaphore()
    for d in range(1, n):
        pl.semaphore_signal(barrier, inc=1, device_id={"fs": (f + d) % n}, device_id_type=MESH)
    for d in range(1, nt):
        pl.semaphore_signal(barrier, inc=1, device_id={"tp": (t + d) % nt}, device_id_type=MESH)

    wq_all[z, y] = wq_ref[...].astype(BF16)
    wo_all[z, y] = wo_ref[...].astype(BF16)
    for c in own:
        c.wait()
    pl.semaphore_wait(barrier, n - 1 + nt - 1)

    started = []

    def send(src, dst, device):
        k = len(started)
        c = pltpu.make_async_remote_copy(
            src_ref=src, dst_ref=dst, send_sem=send_sem.at[k], recv_sem=recv_sem.at[k],
            device_id=device, device_id_type=MESH,
        )
        c.start()
        started.append(c)
        return c

    def to_z(d):
        return {"fs": ((z + d) % nz) * ny + y}

    def to_y(d):
        return {"fs": z * ny + (y + d) % ny}

    def z_send(block, ds):
        return {d: send(block(z), block(z), to_z(d)) for d in ds}

    def y_send(block, back):
        zz = (z + nz - back) % nz
        return [send(block(zz), block(zz), to_y(d)) for d in range(1, ny)]

    fac_block = lambda zz: fac.at[zz, y, :, half]
    wq_block = lambda zz: wq_all.at[zz, y]
    wo_block = lambda zz: wo_all.at[zz, y]
    dq_block = lambda zz: dq_all.at[zz, y]
    do_block = lambda zz: do_all.at[zz, y]

    far = range(1, nz)
    fac_z = z_send(fac_block, far)
    fac_y = y_send(fac_block, 0)
    early = far[: max(1, len(far) - 1)]
    w_z = {}
    for d in early:
        w_z[d] = (send(wo_block(z), wo_block(z), to_z(d)), send(wq_block(z), wq_block(z), to_z(d)))
    w_y = y_send(wo_block, 0) + y_send(wq_block, 0)

    grad_o[...] = jnp.zeros_like(grad_o)
    grad_q[...] = jnp.zeros_like(grad_q)

    def product(k, pair, sem, out):
        for c in load(k, pair, sem):
            c.wait()
        rows = pl.ds(pl.multiple_of(k * step, step), step)
        out[...] += over_rows(pair[1][1][rows, :], pair[0][1][rows, :])

    @pl.loop(0, CHUNKS // 2)
    def _(k):
        product(k, pair_o, 0, grad_o)

    for d in far:
        fac_z[d].wait_recv()
        fac_y += y_send(fac_block, d)
    swap = [send(fac.at[:, y, :, half], fac.at[:, y, :, half], {"tp": twin})]

    @pl.loop(CHUNKS // 2, CHUNKS)
    def _(k):
        product(k, pair_o, 0, grad_o)

    for c in fac_y:
        c.wait_recv()
    for d in range(1, ny):
        other = fac.at[:, (y + ny - d) % ny, :, half]
        swap.append(send(other, other, {"tp": twin}))

    @pl.loop(0, CHUNKS)
    def _(k):
        product(k, pair_q, 2, grad_q)

    for c in swap:
        c.wait_recv()

    rank = fac.shape[-1]
    block = rank // n

    def project(lo, hi, grad, part):
        factor = fac[:, :, lo:hi, :].reshape(n * (hi - lo), rank)
        g = grad[...]
        top = g.astype(BF16)
        rest = (g - top.astype(F32)).astype(BF16)
        dims = (((0,), (1,)), ((), ()))
        low = lax.dot_general(factor, top, dims, preferred_element_type=F32)
        low += lax.dot_general(factor, rest, dims, preferred_element_type=F32)
        low *= inv_root
        for i in range(nz):
            for j in range(ny):
                at = (i * ny + j) * block
                part[i, j] = low[at:at + block, :]

    matrices = (
        (rq, fac.shape[2], grad_o, part_o, yin_o, acc_o, zout_o, zin_o),
        (0, rq, grad_q, part_q, yin_q, acc_q, zout_q, zin_q),
    )
    y_in = []
    for lo, hi, grad, part, yin, acc, zout, zin in matrices:
        project(lo, hi, grad, part)
        copies = []
        for d in range(1, ny):
            yy = (y + d) % ny
            acc_send = yin.at[d - 1]
            for i in range(nz):
                yin[ny - 1 + d - 1, i] = part[i, yy].astype(BF16)
            copies.append(send(yin.at[ny - 1 + d - 1], acc_send, to_y(d)))
        y_in.append(copies)

    z_in = []
    for (lo, hi, grad, part, yin, acc, zout, zin), copies in zip(matrices, y_in):
        for i in range(nz):
            acc[i] = part[i, y]
        for d, c in enumerate(copies):
            c.wait_recv()
            for i in range(nz):
                acc[i] += yin[d, i].astype(F32)
        copies = []
        for d in far:
            zout[d - 1] = acc[(z + d) % nz].astype(BF16)
            copies.append(send(zout.at[d - 1], zin.at[d - 1], to_z(d)))
        z_in.append(copies)

    for d in far:
        if d not in w_z:
            w_z[d] = (send(wo_block(z), wo_block(z), to_z(d)), send(wq_block(z), wq_block(z), to_z(d)))

    def forward_weights(d):
        w_z[d][0].wait_recv()
        w_z[d][1].wait_recv()
        return y_send(wo_block, d) + y_send(wq_block, d)

    w_y += forward_weights(1) if nz > 1 else []

    sides = (
        (matrices[0], z_in[0], om_ref, os_ref, low_o, do_all, 1),
        (matrices[1], z_in[1], qm_ref, qs_ref, low_q, dq_all, 0),
    )
    d_z = []
    d_y = []
    for (_, _, _, _, _, acc, _, zin), copies, mean_ref, square_ref, low_ref, d_all, slot in sides:
        low = acc[z]
        for d, c in zip(far, copies):
            c.wait_recv()
            low += zin[d - 1].astype(F32)
        low_ref[...] = low
        mean_new = 0.8 * mean_ref[...] + 0.2 * low
        square_new = 0.9 * square_ref[...] + 0.1 * low * low
        direction = mean_new / jnp.sqrt(square_new)
        d_all[z, y] = direction.astype(BF16)
        tile_tp[0, slot] = jnp.broadcast_to(jnp.sum(direction * direction), tile_tp.shape[2:])
        where = lambda zz, d_all=d_all: d_all.at[zz, y]
        d_z.append((where, z_send(where, far)))
        d_y += y_send(where, 0)

    tiles = [
        send(tile_tp.at[0], tile_tp.at[d], {"tp": (t + d) % nt}) for d in range(1, nt)
    ]
    for c in tiles:
        c.wait_recv()
    tile_fs[0] = jnp.sum(tile_tp[...], axis=0)
    tiles = [
        send(tile_fs.at[0], tile_fs.at[d], {"fs": (f + d) % n}) for d in range(1, n)
    ]
    for d in far:
        for where, copies in d_z:
            copies[d].wait_recv()
            d_y += y_send(where, d)
    for d in far[1:]:
        w_y += forward_weights(d)
    for c in tiles:
        c.wait_recv()
    total[...] = jnp.sum(tile_fs[...], axis=0)
    for c in d_y + w_y:
        c.wait_recv()
    for c in started:
        c.wait_send()


def on_device(
    nz, ny, nt,
    latent_in, query_cot, attn_out, mix_cot, query_weight, output_weight,
    query_factor, output_factor, query_mean, query_square, output_mean, output_square,
):
    n = nz * ny
    tokens = latent_in.shape[0]
    inv_root = 1.0 / math.sqrt(tokens * n)
    rq, cq = query_weight.shape
    ro, co = output_weight.shape
    rank = query_factor.shape[1]
    block = rank // n
    vmem = pl.BlockSpec(memory_space=pltpu.VMEM)
    hbm = pl.BlockSpec(memory_space=pl.ANY)
    copies = copies_of(nz, ny, nt)
    fac, wq, wo, dq, do, low_q, low_o, total = pl.pallas_call(
        functools.partial(fused_kernel, nz, ny, nt, inv_root),
        name="moment_exchange",
        in_specs=[hbm] * 4 + [vmem] * 2 + [hbm] * 2 + [vmem] * 4,
        out_specs=[vmem] * 8,
        out_shape=[
            jax.ShapeDtypeStruct((nz, ny, rq + ro, rank), BF16),
            jax.ShapeDtypeStruct((nz, ny, rq, cq), BF16),
            jax.ShapeDtypeStruct((nz, ny, ro, co), BF16),
            jax.ShapeDtypeStruct((nz, ny, block, cq), BF16),
            jax.ShapeDtypeStruct((nz, ny, block, co), BF16),
            jax.ShapeDtypeStruct((block, cq), F32),
            jax.ShapeDtypeStruct((block, co), F32),
            jax.ShapeDtypeStruct((2, 8, 128), F32),
        ],
        scratch_shapes=[
            pltpu.VMEM(latent_in.shape, BF16),
            pltpu.VMEM(query_cot.shape, BF16),
            pltpu.VMEM(attn_out.shape, BF16),
            pltpu.VMEM(mix_cot.shape, BF16),
            pltpu.VMEM((cq, n * rq), F32),
            pltpu.VMEM((co, n * ro), F32),
            pltpu.VMEM((nz, ny, block, cq), F32),
            pltpu.VMEM((nz, ny, block, co), F32),
            pltpu.VMEM((2 * max(ny - 1, 1), nz, block, cq), BF16),
            pltpu.VMEM((2 * max(ny - 1, 1), nz, block, co), BF16),
            pltpu.VMEM((nz, block, cq), F32),
            pltpu.VMEM((nz, block, co), F32),
            pltpu.VMEM((max(nz - 1, 1), block, cq), BF16),
            pltpu.VMEM((max(nz - 1, 1), block, co), BF16),
            pltpu.VMEM((max(nz - 1, 1), block, cq), BF16),
            pltpu.VMEM((max(nz - 1, 1), block, co), BF16),
            pltpu.VMEM((nt, 2, 8, 128), F32),
            pltpu.VMEM((n, 2, 8, 128), F32),
            pltpu.SemaphoreType.DMA((CHUNKS, 4)),
            pltpu.SemaphoreType.DMA((2,)),
            pltpu.SemaphoreType.DMA((copies,)),
            pltpu.SemaphoreType.DMA((copies,)),
        ],
        compiler_params=pltpu.CompilerParams(
            collective_id=0, has_side_effects=True, vmem_limit_bytes=60 * 1024 * 1024
        ),
    )(
        latent_in, query_cot, attn_out, mix_cot, query_weight, output_weight,
        query_factor, output_factor, query_mean, query_square, output_mean, output_square,
    )

    def finish(factor, factor_all, direction, weight, weight_all, mean, square, low, slot):
        mean_new = 0.8 * mean + 0.2 * low
        square_new = 0.9 * square + 0.1 * low * low
        cols = weight.shape[1]
        scale = 1.0 / jnp.sqrt(total[slot, 0, 0] / (rank * cols * nt) + 0.25)
        direction = direction.reshape(rank, cols)
        step = jnp.dot(factor, direction, preferred_element_type=F32) * scale
        new = weight - 0.02 * step
        full = jnp.dot(factor_all.reshape(-1, rank), direction, preferred_element_type=F32) * scale
        copy = (weight_all.reshape(-1, cols).astype(F32) - 0.02 * full).astype(BF16)
        return step, new, copy, mean_new, square_new

    step_q, new_q, copy_q, mean_q, square_q = finish(
        query_factor, fac[:, :, :rq], dq, query_weight, wq, query_mean, query_square, low_q, 0
    )
    step_o, new_o, copy_o, mean_o, square_o = finish(
        output_factor, fac[:, :, rq:], do, output_weight, wo, output_mean, output_square, low_o, 1
    )
    return (step_q, step_o, new_q, new_o, copy_q, copy_o, mean_q, square_q, mean_o, square_o)


def solution(mesh):
    nz, ny = grid_of(mesh.shape["fs"])
    rows, both, cols = P("fs", None), P("fs", "tp"), P(None, "tp")
    return jax.shard_map(
        functools.partial(on_device, nz, ny, mesh.shape["tp"]),
        mesh=mesh,
        in_specs=(rows, both, rows, both, both, both, rows, rows, both, both, both, both),
        out_specs=(both, both, both, both, cols, cols, both, both, both, both),
        check_vma=False,
    )
```
